32 devices in a mesh: fs: 8 (over z, x), tp: 4 (over y, core).
Axes of the slice: x: 2, y: 2, z: 4, core: 2. Of those that a mesh axis runs over, the one named last changes fastest.
Arguments:
- later_rows: bfloat16 [4096, 2048], P(('fs', 'tp')), may hold values from -6 to 6
- earlier_rows: bfloat16 [4096, 2048], P(('fs', 'tp')), may hold values from -6 to 6
- cotangent: bfloat16 [4096, 2048], P(('fs', 'tp')), may hold values from -6 to 6
- up_weight: bfloat16 [2048, 4096], P('fs', 'tp'), may hold values from -0.125 to 0.125
- down_weight: bfloat16 [2048, 4096], P('fs', 'tp'), may hold values from -0.09375 to 0.09375
- up_total: float32 [2048, 4096], P('fs', 'tp'), may hold values from -6 to 6
- down_total: float32 [2048, 4096], P('fs', 'tp'), may hold values from -6 to 6
Outputs:
- later_out: bfloat16 [4096, 2048], P(('fs', 'tp'))
- earlier_grad: bfloat16 [4096, 2048], P(('fs', 'tp'))
- up_updated: float32 [2048, 4096], P('fs', 'tp')
- down_updated: float32 [2048, 4096], P('fs', 'tp')
The draws below stay inside these ranges and needn't reach their ends.
All inputs are finite; a program needn't handle non-finite values.
Results may differ from the reference program's by a relative error of at most 0.015.
Values may be sent and summed in bfloat16 or wider, within the bound.
A program may use at most 128 MiB of HBM per device.

```python
import math
import jax
import jax.numpy as jnp
from jax import lax

D = 2048
FF = 4096
TOKENS = 4096
FF_TP = 1024
N_TP = 4


def spiked(drawn, rng, source, target, shards_of, factor):
    def block_of(position):
        return (jnp.arange(drawn.shape[position]) // (drawn.shape[position] // shards_of)).reshape((-1,) + (1,) * (drawn.ndim - 1 - position))

    one_side = jax.random.permutation(rng, shards_of)[block_of(target)]
    far = (block_of(target) + shards_of // 2) % shards_of
    return jnp.where((block_of(source) == one_side) | (block_of(source) == far), factor * drawn, drawn)


def steps_of(rng, dims, split, low, largest):
    def one(axis_at, parts):
        steps = jax.random.uniform(jax.random.fold_in(jax.random.fold_in(rng, 6), axis_at), (parts,), jnp.float32, low / len(split), largest / len(split))
        return jnp.repeat(jnp.exp(steps), dims[axis_at] // parts).reshape((-1,) + (1,) * (len(dims) - axis_at - 1))

    level = one(*split[0])
    for cut in split[1:]:
        level = level * one(*cut)
    return level


def scatter_about(key, extent, width, reach, shards=(), kind=jnp.bfloat16):
    loudness = steps_of(key, extent, shards, -0.22, 0.18) if shards else 1.0
    array = jax.random.normal(key, extent, jnp.float32) * width * loudness
    return jnp.minimum(jnp.maximum(array, -reach), reach).astype(kind)


def noise_with(stream_key, dims, width, reach, shards, heavy, kind=jnp.bfloat16):
    entries = width * jax.random.normal(stream_key, dims, jnp.float32)
    if shards:
        entries = entries * steps_of(stream_key, dims, shards, -0.22, 0.18)
    return jnp.clip(spiked(entries, jax.random.fold_in(stream_key, 3), *heavy), -reach, reach).astype(kind)


def setup_inputs(seed: int = 0) -> dict:
    keys = jax.random.split(jax.random.key(seed), 8)
    return {
        "later_rows": scatter_about(keys[0], (TOKENS, D), 1.0, 6.0, ((0, 32),)),
        "earlier_rows": scatter_about(keys[1], (TOKENS, D), 1.0, 6.0, ((0, 32),)),
        "cotangent": noise_with(keys[2], (TOKENS, D), 1.0, 6.0, ((0, 32),), (0, 1, 32, 2.75)),
        "up_weight": scatter_about(keys[3], (D, FF), D ** -0.5, 0.125, ((0, 8), (1, 4))),
        "down_weight": scatter_about(keys[4], (D, FF), FF ** -0.5, 0.09375, ((0, 8), (1, 4))),
        "up_total": scatter_about(keys[5], (D, FF), 1.0, 6.0, ((0, 8), (1, 4)), jnp.float32),
        "down_total": scatter_about(keys[6], (D, FF), 1.0, 6.0, ((0, 8), (1, 4)), jnp.float32),
    }


def blocked_sum(left, right):

    def one_block(carry, index):
        start = (index * FF_TP).astype(jnp.int32)
        left_block = lax.dynamic_slice_in_dim(left, start, FF_TP, 1)
        right_block = lax.dynamic_slice_in_dim(right, start, FF_TP, 1)
        partial_value = lax.dot_general(left_block, right_block, (((1,), (1,)), ((), ())), preferred_element_type=jnp.float32)
        rounded = lax.optimization_barrier(partial_value.astype(jnp.bfloat16))
        return (carry + rounded.astype(jnp.float32), None)
    init = jnp.zeros((left.shape[0], right.shape[0]), jnp.float32)
    total, _ = lax.scan(one_block, init, jnp.arange(N_TP, dtype=jnp.int32))
    return total

def reference(later_rows, earlier_rows, cotangent, up_weight, down_weight, up_total, down_total):
    later_pre = jnp.dot(later_rows, up_weight, preferred_element_type=jnp.float32)
    later_relu = jnp.maximum(later_pre, 0.0)
    later_hidden = (later_relu * later_relu).astype(jnp.bfloat16)
    later_out = blocked_sum(later_hidden, down_weight).astype(jnp.bfloat16)
    earlier_pre = jnp.dot(earlier_rows, up_weight, preferred_element_type=jnp.float32)
    earlier_relu = jnp.maximum(earlier_pre, 0.0)
    earlier_hidden = (earlier_relu * earlier_relu).astype(jnp.bfloat16)
    hidden_grad = jnp.dot(cotangent, down_weight, preferred_element_type=jnp.float32)
    pre_grad = (2.0 * earlier_relu * hidden_grad).astype(jnp.bfloat16)
    earlier_grad = blocked_sum(pre_grad, up_weight).astype(jnp.bfloat16)
    factor = 1.0 / math.sqrt(TOKENS)
    up_term = jnp.dot(earlier_rows.T, pre_grad, preferred_element_type=jnp.float32)
    down_term = jnp.dot(cotangent.T, earlier_hidden, preferred_element_type=jnp.float32)
    up_updated = up_total + up_term * factor
    down_updated = down_total + down_term * factor
    return (later_out, earlier_grad, up_updated, down_updated)
```

```python
import functools
import math

import jax
import jax.numpy as jnp
from jax import lax
from jax.experimental import pallas as pl
from jax.experimental.pallas import tpu as pltpu
from jax.sharding import PartitionSpec as P

MESH = pl.DeviceIdType.MESH
BF16 = jnp.bfloat16
F32 = jnp.float32


def columns_of(n):
    best = 1
    for x in range(1, n + 1):
        if n % x == 0 and 2 * x * x <= n and (n // x) % 2 == 0:
            best = x
    return best


def ring_to_fs(p, n, x_size):
    if x_size == 1:
        return p
    z_size, wide = n // x_size, x_size - 1
    body = z_size * wide
    z, r = p // wide, p % wide
    x = 1 + jnp.where(z % 2 == 0, r, wide - 1 - r)
    back = z_size - 1 - (p - body)
    return jnp.where(p < body, z * x_size + x, back * x_size)


def fs_to_ring(f, n, x_size):
    if x_size == 1:
        return f
    z_size, wide = n // x_size, x_size - 1
    z, x = f // x_size, f % x_size
    r = jnp.where(z % 2 == 0, x - 1, x_size - 1 - x)
    return jnp.where(x == 0, z_size * wide + z_size - 1 - z, z * wide + r)


def kernel(n, m, factor,
           later_ref, earlier_ref, cot_ref, up_ref, down_ref, up_tot_ref, down_tot_ref,
           later_out, earlier_out, up_out, down_out,
           tok, wts, acc, hid, grads, rbuf, part, dbuf, ybuf,
           ty_s, ty_r, td_s, td_r, w_s, w_r, g_s, g_r, od_s, od_r, oy_s, oy_r):
    rows_dev, depth = later_ref.shape
    blk, width = up_ref.shape
    rows = rows_dev * m
    half, y_size = n // 2, m // 2
    aligned = blk % 128 == 0
    fs, tp = lax.axis_index("fs"), lax.axis_index("tp")
    x_size = columns_of(n)
    pos = fs_to_ring(fs, n, x_size)
    y, c = tp // 2, tp % 2

    def at_ring(p):
        return ring_to_fs((p + 2 * n) % n, n, x_size)

    right = {"fs": at_ring(pos + 1), "tp": tp}
    left = {"fs": at_ring(pos - 1), "tp": tp}
    mate = {"fs": fs, "tp": y * 2 + 1 - c}
    y_next = {"fs": fs, "tp": ((y + 1) % y_size) * 2 + c}
    y_prev = {"fs": fs, "tp": ((y + y_size - 1) % y_size) * 2 + c}

    barrier = pltpu.get_barrier_semaphore()
    for other in (right, left, mate, y_next, y_prev):
        pl.semaphore_signal(barrier, inc=1, device_id=other, device_id_type=MESH)
    pl.semaphore_wait(barrier, 5)

    def remote(src, dst, send, recv, to):
        return pltpu.make_async_remote_copy(
            src_ref=src, dst_ref=dst, send_sem=send, recv_sem=recv, device_id=to, device_id_type=MESH)

    def wrows(a, f):
        return wts.at[a, pl.ds(pl.multiple_of(f * blk, blk), blk), :]

    def trows(a, t):
        return tok.at[a, pl.ds(pl.multiple_of(t * rows_dev, rows_dev), rows_dev), :]

    own_w, own_t = (up_ref, down_ref), (earlier_ref, cot_ref, later_ref)

    arr_of, sign_of = (0, 1, 1, 0), (1, -1, 1, -1)

    def w_copy(k, s, first=False):
        f = at_ring(pos - sign_of[k] * s)
        src = own_w[arr_of[k]] if first else wrows(arr_of[k], f)
        return remote(src, wrows(arr_of[k], f), w_s.at[k, s], w_r.at[k, s], right if sign_of[k] > 0 else left)

    def ty_copy(a, s, first=False):
        t = ((y + y_size - s) % y_size) * 2 + c
        return remote(own_t[a] if first else trows(a, t), trows(a, t), ty_s.at[a, s], ty_r.at[a, s], y_next)

    def td_copy(a, s, first=False):
        t = ((y + y_size - s) % y_size) * 2 + c
        return remote(own_t[a] if first else trows(a, t), trows(a, t), td_s.at[a, s], td_r.at[a, s], mate)

    for k in range(4):
        if half - (k >= 2) > 0:
            w_copy(k, 0, True).start()
    for a in range(3):
        if y_size > 1:
            ty_copy(a, 0, True).start()
    for a in range(3):
        td_copy(a, 0, True).start()

    def put(dst, dst_row, src, count):
        step = math.gcd(count, 64)

        @pl.loop(0, count // step)
        def _(i):
            o = pl.multiple_of(i * step, step)
            dst[pl.ds(pl.multiple_of(dst_row + o, step), step), :] = src[pl.ds(o, step), :]

    for a in range(2):
        put(wts.at[a], fs * blk, own_w[a], blk)
    for a in range(3):
        put(tok.at[a], tp * rows_dev, own_t[a], rows_dev)

    tile = math.gcd(width, 256)

    def multiply(a, w, col, size, clear):
        @pl.loop(0, width // tile)
        def _(j):
            o = pl.ds(pl.multiple_of(j * tile, tile), tile)
            got = jnp.dot(tok[a, :, col], wts[w, size, o], preferred_element_type=F32)
            if clear:
                acc[a, :, o] = got
            else:
                acc[a, :, o] += got

    def use(w, f, clear=False):
        if not aligned:
            return
        o = pl.ds(pl.multiple_of(f * blk, blk), blk)
        for a in ((0, 2) if w == 0 else (1,)):
            multiply(a, w, o, o, clear)

    def hop(s, present, go, compute=True):
        for k in present:
            w_copy(k, s - 1).wait_recv()
            if k in go:
                w_copy(k, s).start()
        if compute:
            for k in present:
                use(arr_of[k], at_ring(pos - sign_of[k] * s))

    def streams(s):
        return (0, 1, 2, 3) if s < half else (0, 1)

    def onward(s):
        return tuple(k for k in range(4) if s < half - (k >= 2))

    hop(1, streams(1), onward(1), compute=False)
    for s in range(1, y_size):
        for a in range(3):
            ty_copy(a, s - 1).wait_recv()
            if s < y_size - 1:
                ty_copy(a, s).start()
            td_copy(a, s).start()
    for s in range(y_size):
        for a in range(3):
            td_copy(a, s).wait_recv()
    for w in range(2):
        use(w, fs, True)
    for k in streams(1):
        use(arr_of[k], at_ring(pos - sign_of[k]))
    if half - 2 > 1:
        @pl.loop(2, half - 1)
        def _(s):
            hop(s, (0, 1, 2, 3), (0, 1, 2, 3))
    if half - 1 > 1:
        hop(half - 1, streams(half - 1), onward(half - 1))
    if half > 1:
        hop(half, streams(half), ())
    if not aligned:
        full = pl.ds(0, depth)
        for a, w in ((0, 0), (1, 1), (2, 0)):
            multiply(a, w, full, full, True)

    step_r = math.gcd(rows, 32)

    @pl.loop(0, rows // step_r)
    def _(i):
        o = pl.ds(pl.multiple_of(i * step_r, step_r), step_r)
        relu = jnp.maximum(acc[0, o, :], 0.0)
        hid[0, o, :] = (2.0 * relu * acc[1, o, :]).astype(BF16)
        hid[1, o, :] = (relu * relu).astype(BF16)

    def term(a, row, size):
        @pl.loop(0, width // tile)
        def _(j):
            o = pl.ds(pl.multiple_of(j * tile, tile), tile)
            grads[a, pl.ds(row, size), o] = lax.dot_general(
                tok[a, :, pl.ds(row, size)], hid[a, :, o], (((0,), (0,)), ((), ())),
                preferred_element_type=F32).astype(BF16)

    def block_term(a, p):
        term(a, pl.multiple_of(at_ring(p) * blk, blk), blk)

    def g_copy(k, s):
        d = half - (k >= 2) - s
        f = at_ring(pos + sign_of[k] * d)
        src = grads.at[arr_of[k], pl.ds(pl.multiple_of(f * blk, blk), blk), :]
        return remote(src, rbuf.at[k, s], g_s.at[k, s], g_r.at[k, s], right if sign_of[k] > 0 else left)

    def add_rows(dst, dst_row, src, count):
        step = math.gcd(count, 32)

        @pl.loop(0, count // step)
        def _(i):
            o = pl.multiple_of(i * step, step)
            at = pl.ds(pl.multiple_of(dst_row + o, step), step)
            dst[at, :] = (dst[at, :].astype(F32) + src[pl.ds(o, step), :].astype(F32)).astype(BF16)

    def g_step(s, which):
        for k in which:
            g_copy(k, s - 1).wait_recv()
            f = at_ring(pos + sign_of[k] * (half - (k >= 2) - s))
            add_rows(grads.at[arr_of[k]], f * blk, rbuf.at[k, s - 1], blk)
            g_copy(k, s).start()

    if not aligned:
        wide = math.gcd(depth, 256)
        for a in range(2):
            @pl.loop(0, depth // wide)
            def _(i):
                term(a, pl.multiple_of(i * wide, wide), wide)
    for k in range(4):
        d = half - (k >= 2)
        if d > 0:
            if aligned:
                block_term(arr_of[k], pos + sign_of[k] * d)
            g_copy(k, 0).start()
    if aligned:
        if half > 1:
            @pl.loop(0, half - 1)
            def _(i):
                d = half - 1 - i
                block_term(0, pos + d)
                block_term(1, pos - d)
        if half > 2:
            @pl.loop(0, half - 2)
            def _(i):
                d = half - 2 - i
                block_term(1, pos + d)
                block_term(0, pos - d)
        for a in range(2):
            block_term(a, pos)

    @pl.loop(0, rows // step_r)
    def _(i):
        o = pl.ds(pl.multiple_of(i * step_r, step_r), step_r)
        relu = jnp.maximum(acc[2, o, :], 0.0)
        hid[2, o, :] = (relu * relu).astype(BF16)

    wide_d = math.gcd(depth, 256)

    def partial(a, h, w):
        @pl.loop(0, depth // wide_d)
        def _(j):
            o = pl.ds(pl.multiple_of(j * wide_d, wide_d), wide_d)
            part[a, :, o] = lax.dot_general(
                hid[h], wts[w, o, :], (((1,), (1,)), ((), ())), preferred_element_type=F32).astype(BF16)

    def prow(yy, cc):
        return pl.multiple_of((yy * 2 + cc) * rows_dev, rows_dev)

    def od_copy(a, yy):
        return remote(part.at[a, pl.ds(prow(yy, 1 - c), rows_dev), :], dbuf.at[a, yy],
                      od_s.at[a, yy], od_r.at[a, yy], mate)

    def oy_copy(a, s):
        t = (y + y_size - 1 - s) % y_size
        return remote(part.at[a, pl.ds(prow(t, c), rows_dev), :], ybuf.at[a, s],
                      oy_s.at[a, s], oy_r.at[a, s], y_next)

    for a, h, w in ((0, 0, 0), (1, 2, 1)):
        partial(a, h, w)
        for yy in range(y_size):
            od_copy(a, yy).start()

    if half > 1:
        g_step(1, onward(1))
    for a in range(2):
        for yy in range(y_size):
            od_copy(a, yy).wait_recv()
            add_rows(part.at[a], prow(yy, c), dbuf.at[a, yy], rows_dev)
        if y_size > 1:
            oy_copy(a, 0).start()
    if half - 1 > 2:
        @pl.loop(2, half - 1)
        def _(s):
            g_step(s, (0, 1, 2, 3))
    for s in range(1, y_size):
        for a in range(2):
            oy_copy(a, s - 1).wait_recv()
            t = (y + y_size - 1 - s) % y_size
            add_rows(part.at[a], prow(t, c), ybuf.at[a, s - 1], rows_dev)
            if s < y_size - 1:
                oy_copy(a, s).start()
    put_own = ((earlier_out, 0), (later_out, 1))
    for out, a in put_own:
        out[...] = part[a, pl.ds(prow(y, c), rows_dev), :]
    if half - 1 >= 2:
        g_step(half - 1, (0, 1))

    ends = [(k, half - 1 - (k >= 2)) for k in range(4)]
    for k, s in ends:
        if s >= 0:
            g_copy(k, s).wait_recv()
    step_b = math.gcd(blk, 32)
    for a, out, tot in ((0, up_out, up_tot_ref), (1, down_out, down_tot_ref)):
        @pl.loop(0, blk // step_b)
        def _(i):
            lo = pl.multiple_of(i * step_b, step_b)
            o = pl.ds(lo, step_b)
            got = grads[a, pl.ds(pl.multiple_of(fs * blk + lo, step_b), step_b), :].astype(F32)
            for k, s in ends:
                if arr_of[k] == a and s >= 0:
                    got += rbuf[k, s, o, :].astype(F32)
            out[o, :] = tot[o, :] + got * factor

    for k in range(4):
        for s in range(half - (k >= 2)):
            w_copy(k, s).wait_send()
            g_copy(k, s).wait_send()
    for a in range(3):
        for s in range(y_size):
            if s < y_size - 1:
                ty_copy(a, s).wait_send()
            td_copy(a, s).wait_send()
    for a in range(2):
        for yy in range(y_size):
            od_copy(a, yy).wait_send()
        for s in range(y_size - 1):
            oy_copy(a, s).wait_send()


def body(n, m, later_rows, earlier_rows, cotangent, up_weight, down_weight, up_total, down_total):
    rows_dev, depth = later_rows.shape
    blk, width = up_weight.shape
    rows, half, y_size = rows_dev * m, n // 2, m // 2
    factor = 1.0 / math.sqrt(rows * n)
    dma = pltpu.SemaphoreType.DMA
    vmem = pl.BlockSpec(memory_space=pltpu.VMEM)
    sums = max(y_size - 1, 1)
    return pl.pallas_call(
        functools.partial(kernel, n, m, factor),
        out_shape=(
            jax.ShapeDtypeStruct((rows_dev, depth), BF16),
            jax.ShapeDtypeStruct((rows_dev, depth), BF16),
            jax.ShapeDtypeStruct((blk, width), F32),
            jax.ShapeDtypeStruct((blk, width), F32),
        ),
        in_specs=[vmem] * 7,
        out_specs=(vmem,) * 4,
        scratch_shapes=[
            pltpu.VMEM((3, rows, depth), BF16),
            pltpu.VMEM((2, depth, width), BF16),
            pltpu.VMEM((3, rows, width), F32),
            pltpu.VMEM((3, rows, width), BF16),
            pltpu.VMEM((2, depth, width), BF16),
            pltpu.VMEM((4, half, blk, width), BF16),
            pltpu.VMEM((2, rows, depth), BF16),
            pltpu.VMEM((2, y_size, rows_dev, depth), BF16),
            pltpu.VMEM((2, sums, rows_dev, depth), BF16),
            dma((3, y_size)), dma((3, y_size)), dma((3, y_size)), dma((3, y_size)),
            dma((4, half)), dma((4, half)), dma((4, half)), dma((4, half)),
            dma((2, y_size)), dma((2, y_size)), dma((2, sums)), dma((2, sums)),
        ],
        compiler_params=pltpu.CompilerParams(
            collective_id=0, has_side_effects=True, vmem_limit_bytes=67043328
        ),
        name="feed_forward_step",
    )(later_rows, earlier_rows, cotangent, up_weight, down_weight, up_total, down_total)


def solution(mesh):
    return jax.shard_map(
        functools.partial(body, mesh.shape["fs"], mesh.shape["tp"]),
        mesh=mesh,
        in_specs=(
            P(("fs", "tp"), None),
            P(("fs", "tp"), None),
            P(("fs", "tp"), None),
            P("fs", "tp"),
            P("fs", "tp"),
            P("fs", "tp"),
            P("fs", "tp"),
        ),
        out_specs=(P(("fs", "tp"), None), P(("fs", "tp"), None), P("fs", "tp"), P("fs", "tp")),
        check_vma=False,
    )
```

```python
import functools
import math

import jax
import jax.numpy as jnp
from jax import lax
from jax.experimental import pallas as pl
from jax.experimental.pallas import tpu as pltpu
from jax.sharding import PartitionSpec as P

MESH = pl.DeviceIdType.MESH
BF16 = jnp.bfloat16
F32 = jnp.float32


def columns_of(n):
    best = 1
    for x in range(1, n + 1):
        if n % x == 0 and 2 * x * x <= n and (n // x) % 2 == 0:
            best = x
    return best


def ring_to_fs(p, n, x_size):
    if x_size == 1:
        return p
    z_size, wide = n // x_size, x_size - 1
    body = z_size * wide
    z, r = p // wide, p % wide
    x = 1 + jnp.where(z % 2 == 0, r, wide - 1 - r)
    back = z_size - 1 - (p - body)
    return jnp.where(p < body, z * x_size + x, back * x_size)


def fs_to_ring(f, n, x_size):
    if x_size == 1:
        return f
    z_size, wide = n // x_size, x_size - 1
    z, x = f // x_size, f % x_size
    r = jnp.where(z % 2 == 0, x - 1, x_size - 1 - x)
    return jnp.where(x == 0, z_size * wide + z_size - 1 - z, z * wide + r)


def kernel(n, m, parts,
           later_ref, earlier_ref, cot_ref, up_ref, down_ref,
           later_out, earlier_out, up_out, down_out,
           tok, wts, acc, hid, grads, rbuf, part, dbuf, ybuf,
           ty_s, ty_r, td_s, td_r, w_s, w_r, g_s, g_r, od_s, od_r, oy_s, oy_r):
    rows_dev, depth = later_ref.shape
    blk, width = up_ref.shape
    rows = rows_dev * m
    half, y_size = n // 2, m // 2
    aligned = blk % 128 == 0
    wide_q = width // parts
    fs, tp = lax.axis_index("fs"), lax.axis_index("tp")
    x_size = columns_of(n)
    pos = fs_to_ring(fs, n, x_size)
    y, c = tp // 2, tp % 2

    def at_ring(p):
        return ring_to_fs((p + 2 * n) % n, n, x_size)

    right = {"fs": at_ring(pos + 1), "tp": tp}
    left = {"fs": at_ring(pos - 1), "tp": tp}
    mate = {"fs": fs, "tp": y * 2 + 1 - c}
    y_next = {"fs": fs, "tp": ((y + 1) % y_size) * 2 + c}
    y_prev = {"fs": fs, "tp": ((y + y_size - 1) % y_size) * 2 + c}

    barrier = pltpu.get_barrier_semaphore()
    for other in (right, left, mate, y_next, y_prev):
        pl.semaphore_signal(barrier, inc=1, device_id=other, device_id_type=MESH)
    pl.semaphore_wait(barrier, 5)

    def remote(src, dst, send, recv, to):
        return pltpu.make_async_remote_copy(
            src_ref=src, dst_ref=dst, send_sem=send, recv_sem=recv, device_id=to, device_id_type=MESH)

    def trows(a, t):
        return tok.at[a, pl.ds(pl.multiple_of(t * rows_dev, rows_dev), rows_dev), :]

    own_w, own_t = (up_ref, down_ref), (earlier_ref, cot_ref, later_ref)

    arr_of, sign_of = (0, 1, 1, 0), (1, -1, 1, -1)

    def cut(q):
        return pl.ds(q * wide_q, wide_q)

    def w_copy(k, s, q, first=False):
        f = at_ring(pos - sign_of[k] * s)
        there = wts.at[arr_of[k], pl.ds(pl.multiple_of(f * blk, blk), blk), cut(q)]
        src = own_w[arr_of[k]].at[:, cut(q)] if first else there
        return remote(src, there, w_s.at[k, s, q], w_r.at[k, s, q], right if sign_of[k] > 0 else left)

    def ty_copy(a, s, first=False):
        t = ((y + y_size - s) % y_size) * 2 + c
        return remote(own_t[a] if first else trows(a, t), trows(a, t), ty_s.at[a, s], ty_r.at[a, s], y_next)

    def td_copy(a, s, first=False):
        t = ((y + y_size - s) % y_size) * 2 + c
        return remote(own_t[a] if first else trows(a, t), trows(a, t), td_s.at[a, s], td_r.at[a, s], mate)

    every = tuple((k, q) for pair in ((0, 1), (2, 3)) for q in range(parts) for k in pair)
    longs = tuple((k, q) for k, q in every if k < 2)
    for k, q in every:
        w_copy(k, 0, q, True).start()
    for a in range(3):
        if y_size > 1:
            ty_copy(a, 0, True).start()
    for a in range(3):
        td_copy(a, 0, True).start()

    def put(dst, dst_row, src, count):
        step = math.gcd(count, 64)

        @pl.loop(0, count // step)
        def _(i):
            o = pl.multiple_of(i * step, step)
            dst[pl.ds(pl.multiple_of(dst_row + o, step), step), :] = src[pl.ds(o, step), :]

    for a in range(2):
        put(wts.at[a], fs * blk, own_w[a], blk)
    for a in range(3):
        put(tok.at[a], tp * rows_dev, own_t[a], rows_dev)

    tile = math.gcd(wide_q, 256)

    def multiply(a, w, rows_w, clear, q=None):
        first, count = (0, width) if q is None else (q * wide_q, wide_q)

        @pl.loop(0, count // tile)
        def _(j):
            o = pl.ds(pl.multiple_of(first + j * tile, tile), tile)
            got = jnp.dot(tok[a, :, rows_w], wts[w, rows_w, o], preferred_element_type=F32)
            if clear:
                acc[a, :, o] = got
            else:
                acc[a, :, o] += got

    def use(w, f, clear=False, q=None):
        if not aligned:
            return
        o = pl.ds(pl.multiple_of(f * blk, blk), blk)
        for a in ((0, 2) if w == 0 else (1,)):
            multiply(a, w, o, clear, q)

    def forward(s, present, go):
        for k, q in present:
            w_copy(k, s - 1, q).wait_recv()
            if (k, q) in go:
                w_copy(k, s, q).start()

    def use_step(s):
        for k in range(4):
            use(arr_of[k], at_ring(pos - sign_of[k] * s))

    forward(1, every, every if half > 2 else longs)
    for s in range(1, y_size):
        for a in range(3):
            ty_copy(a, s - 1).wait_recv()
            if s < y_size - 1:
                ty_copy(a, s).start()
            td_copy(a, s).start()
    for s in range(y_size):
        for a in range(3):
            td_copy(a, s).wait_recv()
    for w in range(2):
        use(w, fs, True)
    if half > 3:
        @pl.loop(2, half - 1)
        def _(s):
            forward(s, every, every)
            use_step(s - 1)
    if half > 2:
        forward(half - 1, every, longs)
        use_step(half - 2)
    use_step(half - 1)

    step_r = math.gcd(rows, 32)

    def activate(q):
        @pl.loop(0, rows // step_r)
        def _(i):
            o = pl.ds(pl.multiple_of(i * step_r, step_r), step_r)
            relu = jnp.maximum(acc[0, o, cut(q)], 0.0)
            hid[0, o, cut(q)] = (2.0 * relu * acc[1, o, cut(q)]).astype(BF16)
            hid[1, o, cut(q)] = (relu * relu).astype(BF16)

    def term(a, row, size, q=None):
        first, count = (0, width) if q is None else (q * wide_q, wide_q)

        @pl.loop(0, count // tile)
        def _(j):
            o = pl.ds(pl.multiple_of(first + j * tile, tile), tile)
            grads[a, pl.ds(row, size), o] = lax.dot_general(
                tok[a, :, pl.ds(row, size)], hid[a, :, o], (((0,), (0,)), ((), ())),
                preferred_element_type=F32).astype(BF16)

    def block_term(a, p, q=None):
        term(a, pl.multiple_of(at_ring(p) * blk, blk), blk, q)

    def g_copy(k, s, q):
        d = half - (k >= 2) - s
        f = at_ring(pos + sign_of[k] * d)
        src = grads.at[arr_of[k], pl.ds(pl.multiple_of(f * blk, blk), blk), cut(q)]
        return remote(src, rbuf.at[k, s, :, cut(q)], g_s.at[k, s, q], g_r.at[k, s, q],
                      right if sign_of[k] > 0 else left)

    def add_rows(dst, dst_row, src, count, columns=slice(None)):
        step = math.gcd(count, 32)

        @pl.loop(0, count // step)
        def _(i):
            o = pl.multiple_of(i * step, step)
            at = pl.ds(pl.multiple_of(dst_row + o, step), step)
            total = dst[at, columns].astype(F32) + src[pl.ds(o, step), columns].astype(F32)
            dst[at, columns] = total.astype(BF16)

    def g_step(s, which):
        for k, q in which:
            g_copy(k, s - 1, q).wait_recv()
            f = at_ring(pos + sign_of[k] * (half - (k >= 2) - s))
            add_rows(grads.at[arr_of[k]], f * blk, rbuf.at[k, s - 1], blk, cut(q))
            g_copy(k, s, q).start()

    wide = math.gcd(depth, 256)
    for q in range(parts):
        for k in (0, 1):
            w_copy(k, half - 1, q).wait_recv()
            use(arr_of[k], at_ring(pos - sign_of[k] * half), q=q)
        if not aligned:
            full = pl.ds(0, depth)
            for a, w in ((0, 0), (1, 1), (2, 0)):
                multiply(a, w, full, True, q)
        activate(q)
        if not aligned:
            for a in range(2):
                @pl.loop(0, depth // wide)
                def _(i):
                    term(a, pl.multiple_of(i * wide, wide), wide, q)
        for k in (0, 1):
            if aligned:
                block_term(arr_of[k], pos + sign_of[k] * half, q)
            g_copy(k, 0, q).start()
    for k in (2, 3):
        if aligned:
            block_term(arr_of[k], pos + sign_of[k] * (half - 1))
        for q in range(parts):
            g_copy(k, 0, q).start()
    if aligned:
        if half > 1:
            @pl.loop(0, half - 1)
            def _(i):
                d = half - 1 - i
                block_term(0, pos + d)
                block_term(1, pos - d)
        if half > 2:
            @pl.loop(0, half - 2)
            def _(i):
                d = half - 2 - i
                block_term(1, pos + d)
                block_term(0, pos - d)
        for a in range(2):
            block_term(a, pos)

    @pl.loop(0, rows // step_r)
    def _(i):
        o = pl.ds(pl.multiple_of(i * step_r, step_r), step_r)
        relu = jnp.maximum(acc[2, o, :], 0.0)
        hid[2, o, :] = (relu * relu).astype(BF16)

    wide_d = math.gcd(depth, 256)

    def partial(a, h, w):
        @pl.loop(0, depth // wide_d)
        def _(j):
            o = pl.ds(pl.multiple_of(j * wide_d, wide_d), wide_d)
            part[a, :, o] = lax.dot_general(
                hid[h], wts[w, o, :], (((1,), (1,)), ((), ())), preferred_element_type=F32).astype(BF16)

    def prow(yy, cc):
        return pl.multiple_of((yy * 2 + cc) * rows_dev, rows_dev)

    def od_copy(a, yy):
        return remote(part.at[a, pl.ds(prow(yy, 1 - c), rows_dev), :], dbuf.at[a, yy],
                      od_s.at[a, yy], od_r.at[a, yy], mate)

    def oy_copy(a, s):
        t = (y + y_size - 1 - s) % y_size
        return remote(part.at[a, pl.ds(prow(t, c), rows_dev), :], ybuf.at[a, s],
                      oy_s.at[a, s], oy_r.at[a, s], y_next)

    def send_partial(a, h, w):
        partial(a, h, w)
        for yy in range(y_size):
            od_copy(a, yy).start()

    send_partial(0, 0, 0)
    g_step(1, every if half > 2 else longs)
    send_partial(1, 2, 1)
    for a in range(2):
        for yy in range(y_size):
            od_copy(a, yy).wait_recv()
            add_rows(part.at[a], prow(yy, c), dbuf.at[a, yy], rows_dev)
        if y_size > 1:
            oy_copy(a, 0).start()
    if half - 1 > 2:
        @pl.loop(2, half - 1)
        def _(s):
            g_step(s, every)
    for s in range(1, y_size):
        for a in range(2):
            oy_copy(a, s - 1).wait_recv()
            t = (y + y_size - 1 - s) % y_size
            add_rows(part.at[a], prow(t, c), ybuf.at[a, s - 1], rows_dev)
            if s < y_size - 1:
                oy_copy(a, s).start()
    put_own = ((earlier_out, 0), (later_out, 1))
    for out, a in put_own:
        out[...] = part[a, pl.ds(prow(y, c), rows_dev), :]
    if half - 1 >= 2:
        g_step(half - 1, longs)

    ends = [(k, half - 1 - (k >= 2)) for k in range(4)]
    for k, q in tuple((k, q) for k, q in every if k >= 2) + longs:
        g_copy(k, ends[k][1], q).wait_recv()
    step_b = math.gcd(blk, 32)
    for a, out in ((0, up_out), (1, down_out)):
        @pl.loop(0, blk // step_b)
        def _(i):
            lo = pl.multiple_of(i * step_b, step_b)
            o = pl.ds(lo, step_b)
            got = grads[a, pl.ds(pl.multiple_of(fs * blk + lo, step_b), step_b), :].astype(F32)
            for k, s in ends:
                if arr_of[k] == a:
                    got += rbuf[k, s, o, :].astype(F32)
            out[o, :] = got.astype(BF16)

    for k, q in every:
        for s in range(half - (k >= 2)):
            w_copy(k, s, q).wait_send()
            g_copy(k, s, q).wait_send()
    for a in range(3):
        for s in range(y_size):
            if s < y_size - 1:
                ty_copy(a, s).wait_send()
            td_copy(a, s).wait_send()
    for a in range(2):
        for yy in range(y_size):
            od_copy(a, yy).wait_send()
        for s in range(y_size - 1):
            oy_copy(a, s).wait_send()


def body(n, m, later_rows, earlier_rows, cotangent, up_weight, down_weight, up_total, down_total):
    rows_dev, depth = later_rows.shape
    blk, width = up_weight.shape
    rows, half, y_size = rows_dev * m, n // 2, m // 2
    factor = 1.0 / math.sqrt(rows * n)
    dma = pltpu.SemaphoreType.DMA
    vmem = pl.BlockSpec(memory_space=pltpu.VMEM)
    sums = max(y_size - 1, 1)
    parts = 2 if width % 256 == 0 else 1
    later_out, earlier_grad, up_term, down_term = pl.pallas_call(
        functools.partial(kernel, n, m, parts),
        out_shape=(
            jax.ShapeDtypeStruct((rows_dev, depth), BF16),
            jax.ShapeDtypeStruct((rows_dev, depth), BF16),
            jax.ShapeDtypeStruct((blk, width), BF16),
            jax.ShapeDtypeStruct((blk, width), BF16),
        ),
        in_specs=[vmem] * 5,
        out_specs=(vmem,) * 4,
        scratch_shapes=[
            pltpu.VMEM((3, rows, depth), BF16),
            pltpu.VMEM((2, depth, width), BF16),
            pltpu.VMEM((3, rows, width), F32),
            pltpu.VMEM((3, rows, width), BF16),
            pltpu.VMEM((2, depth, width), BF16),
            pltpu.VMEM((4, half, blk, width), BF16),
            pltpu.VMEM((2, rows, depth), BF16),
            pltpu.VMEM((2, y_size, rows_dev, depth), BF16),
            pltpu.VMEM((2, sums, rows_dev, depth), BF16),
            dma((3, y_size)), dma((3, y_size)), dma((3, y_size)), dma((3, y_size)),
            *[dma((4, half, parts))] * 4,
            dma((2, y_size)), dma((2, y_size)), dma((2, sums)), dma((2, sums)),
        ],
        compiler_params=pltpu.CompilerParams(
            collective_id=0, has_side_effects=True, vmem_limit_bytes=67043328
        ),
        name="feed_forward_step",
    )(later_rows, earlier_rows, cotangent, up_weight, down_weight)
    up_updated = up_total + up_term.astype(F32) * factor
    down_updated = down_total + down_term.astype(F32) * factor
    return later_out, earlier_grad, up_updated, down_updated


def solution(mesh):
    return jax.shard_map(
        functools.partial(body, mesh.shape["fs"], mesh.shape["tp"]),
        mesh=mesh,
        in_specs=(
            P(("fs", "tp"), None),
            P(("fs", "tp"), None),
            P(("fs", "tp"), None),
            P("fs", "tp"),
            P("fs", "tp"),
            P("fs", "tp"),
            P("fs", "tp"),
        ),
        out_specs=(P(("fs", "tp"), None), P(("fs", "tp"), None), P("fs", "tp"), P("fs", "tp")),
        check_vma=False,
    )
```
